32 devices in a mesh: ep: 8 (over z, x), tp: 4 (over y, core).
Axes of the slice: x: 2, y: 2, z: 4, core: 2. Of those that a mesh axis runs over, the one named last changes fastest.
Arguments:
- tokens: bfloat16 [1024, 2048], P('ep'), may hold values from -16 to 16
- routes: int32 [1024, 2], P('ep'), may hold values from 0 to 7, all different within a row; in each aligned block of 128 rows (0 to 127, 128 to 255, ...) at most 48 rows name the same one
- router: bfloat16 [2048, 8], replicated, may hold values from -0.125 to 0.125
- w_gate: bfloat16 [8, 2048, 2048], P('ep', None, 'tp'), may hold values from -0.125 to 0.125
- w_up: bfloat16 [8, 2048, 2048], P('ep', None, 'tp'), may hold values from -0.125 to 0.125
- w_down: bfloat16 [8, 2048, 2048], P('ep', 'tp'), may hold values from -0.125 to 0.125
- cotangent: bfloat16 [1024, 2048], P('ep'), may hold values from -6 to 6
Outputs:
- grad_tokens: bfloat16 [1024, 2048], P('ep', 'tp')
- grad_router: float32 [2048, 8], P('tp')
- grad_gate: float32 [8, 2048, 2048], P('ep', None, 'tp')
- grad_up: float32 [8, 2048, 2048], P('ep', None, 'tp')
- grad_down: float32 [8, 2048, 2048], P('ep', 'tp')
The draws below stay inside these ranges and needn't reach their ends.
Inputs may be any that keep to these rules, and one draw needn't show every extreme that they name: In each aligned block of 128 rows, no expert is named by more than 48 of the block's routes, a bound that some block reaches; a row names 2 different experts.
All inputs are finite; a program needn't handle non-finite values.
Results may differ from the reference program's by a relative error of at most 0.017.
Values may be sent and summed in bfloat16 or wider, within the bound.
No kernel may reach another device: no remote copies, remote signals or barrier semaphores. Data moves between devices by JAX's collectives and lax.ppermute only.
A program may use at most 128 MiB of HBM per device.

```python
import math
import jax
import jax.numpy as jnp
import numpy as np
from jax import lax

D = 2048
FF = 2048
TOP_K = 2
TOK_DEV = 128
EXPERTS = 8
CAP = 48
TOKENS = 1024
N_EP = 8
N_TP = 4


def draw_tokens(key, part):
    key_rows = jax.random.fold_in(key, 11)
    key_vals = jax.random.fold_in(key, 23)
    values = jax.random.truncated_normal(key_vals, -4.0, 4.0, (TOKENS, D), jnp.float32)
    scales = jnp.exp(jax.random.uniform(key_rows, (TOKENS, 1), jnp.float32, math.log(0.5), math.log(4.0)))
    return (values * scales).astype(jnp.bfloat16)


def level_of(key, shape, shards, smallest, top_value):
    loudness = 1.0
    for axis_at, shards_of in shards:
        draws = jax.random.uniform(jax.random.fold_in(jax.random.fold_in(key, 6), axis_at), (shards_of,), jnp.float32, smallest / len(shards), top_value / len(shards))
        loudness = loudness * jnp.repeat(jnp.exp(draws), shape[axis_at] // shards_of).reshape((-1,) + (1,) * (len(shape) - 1 - axis_at))
    return loudness


def assign_block(rng, own, number, rows, number_of, top, limit, skew):
    order = jax.random.permutation(rng, number_of)
    crowded, common = load_shares(number_of, rows * top, limit, skew, True), load_shares(number_of, rows * top, limit, skew, False)
    places = jnp.arange(number_of)

    def named(tallies, rotation):
        used = int((tallies > 0).sum())
        fixed = max(1, used // 4)
        passed = fixed + (places - fixed + rotation * (used - fixed)) % max(1, number_of - fixed)
        return jnp.zeros((number_of,), jnp.int32).at[order[jnp.where(places < fixed, places, passed)]].set(jnp.asarray(tallies, jnp.int32))

    tallies = jnp.where(number % 4 == 0, named(crowded, number // 4), named(common, number - number // 4 - 1))
    mixed = jax.random.permutation(jax.random.fold_in(own, 3), number_of)
    giver, taker = mixed[0:number_of // 2 * 2:2], mixed[1:number_of // 2 * 2:2]
    slack = jnp.minimum(tallies[giver] - 1, limit - tallies[taker]) // 2
    slack = jnp.where((giver == order[0]) | (taker == order[0]) | (tallies[taker] == 0), 0, jnp.maximum(slack, 0))
    passed = jax.random.randint(jax.random.fold_in(own, 4), (number_of // 2,), 0, 1 << 20) % (slack + 1)
    tallies = tallies.at[giver].add(-passed).at[taker].add(passed)
    items = jnp.searchsorted(jnp.cumsum(tallies), jnp.arange(rows * top), side="right").astype(jnp.int32)
    listing = items.reshape(top, rows).T
    listing = listing[jax.random.permutation(jax.random.fold_in(own, 1), rows)]
    rotation = jax.random.randint(jax.random.fold_in(own, 2), (rows, 1), 0, top)
    return jnp.take_along_axis(listing, (jnp.arange(top)[None, :] + rotation) % top, axis=1)


def load_shares(amount, total, bound, lean, full):
    portions = [(1 << 20) // math.isqrt(standing ** lean) + 1 for standing in range(1, amount + 1)]
    largest = bound if full else min(bound, max(-(-total // amount), total * portions[0] // sum(portions)))
    least = 1 if total - largest >= amount - 1 else 0
    given, rest = [largest] + [least] * (amount - 1), total - largest - least * (amount - 1)
    while rest > 0:
        candidates = [i for i in range(1, amount) if given[i] < largest] or [i for i in range(1, amount) if given[i] < bound]
        whole, budget = sum([portions[i] for i in candidates]), rest
        for i in candidates:
            addition = min(bound - given[i], max(1, budget * portions[i] // whole), rest)
            given[i] = given[i] + addition
            rest = rest - addition
    return np.array(given)


def scatter_about(stream_key, shape, deviation, limit, split=(), kind=jnp.bfloat16):
    array = deviation * jax.random.normal(stream_key, shape, jnp.float32)
    if split:
        array = array * level_of(stream_key, shape, split, -0.22, 0.18)
    return jnp.clip(array, -limit, limit).astype(kind)


def setup_inputs(seed: int = 0) -> dict:
    key_list = jax.random.split(jax.random.key(seed), 8)
    tokens = draw_tokens(jax.random.fold_in(key_list[7], 71), 0)
    routes_keys = jax.random.split(jax.random.fold_in(key_list[1], 1), TOKENS // TOK_DEV)
    routes_turns = jax.random.permutation(jax.random.fold_in(key_list[1], 3), TOKENS // TOK_DEV)
    routes = jax.vmap(lambda own, number: assign_block(jax.random.fold_in(key_list[1], 2), own, number, TOK_DEV, EXPERTS, TOP_K, CAP, 2))(routes_keys, routes_turns).reshape((TOKENS, TOP_K))
    router = scatter_about(key_list[2], (D, EXPERTS), D ** -0.5, 0.125)
    w_gate = scatter_about(key_list[3], (EXPERTS, D, FF), D ** -0.5, 0.125, ((0, 8), (2, 4)))
    w_up = scatter_about(key_list[4], (EXPERTS, D, FF), D ** -0.5, 0.125, ((0, 8), (2, 4)))
    w_down = scatter_about(key_list[5], (EXPERTS, FF, D), FF ** -0.5, 0.125, ((0, 8), (1, 4)))
    cotangent = scatter_about(key_list[6], (TOKENS, D), 1.0, 6.0, ((0, 8),))
    return {"tokens": tokens, "routes": routes, "router": router, "w_gate": w_gate, "w_up": w_up, "w_down": w_down, "cotangent": cotangent}


clamp_limit = 7.0
sig_slope = 1.702


def reference(tokens, routes, router, w_gate, w_up, w_down, cotangent):
    highest = lax.Precision.HIGHEST
    assign_count = TOKENS * TOP_K
    logits = jnp.dot(tokens, router, preferred_element_type=jnp.float32)
    chosen = jnp.take_along_axis(logits, routes, axis=1)
    weights = 1.0 / jnp.sum(jnp.exp(chosen[:, None, :] - chosen[:, :, None]), axis=2)
    scaled = (weights[:, :, None] * cotangent[:, None, :].astype(jnp.float32)).astype(jnp.bfloat16)
    flat_routes = routes.reshape(N_EP, TOK_DEV * TOP_K)
    flat_hot = jax.nn.one_hot(flat_routes, EXPERTS, dtype=jnp.int32)
    earlier = jnp.cumsum(flat_hot, axis=1) - flat_hot
    position = jnp.sum(earlier * flat_hot, axis=2).reshape(-1).astype(jnp.int32)
    block_of = (jnp.arange(assign_count, dtype=jnp.int32) // (TOK_DEV * TOP_K)).astype(jnp.int32)
    slot_table = jnp.full((EXPERTS, N_EP, CAP), assign_count, jnp.int32)
    slot_table = slot_table.at[routes.reshape(-1).astype(jnp.int32), block_of, position].set(
        jnp.arange(assign_count, dtype=jnp.int32))
    slot_table = slot_table.reshape(EXPERTS, N_EP * CAP)
    token_pad = jnp.concatenate([tokens, jnp.zeros((1, D), jnp.bfloat16)], axis=0)
    scaled_pad = jnp.concatenate([scaled.reshape(assign_count, D), jnp.zeros((1, D), jnp.bfloat16)], axis=0)
    group_size = FF // N_TP

    def one_expert(packed):
        slots, gate_w, up_w, down_w = packed
        rows_in = token_pad[slots // TOP_K]
        cot_in = scaled_pad[slots]
        pre_gate = jnp.dot(rows_in, gate_w, preferred_element_type=jnp.float32)
        pre_up = jnp.dot(rows_in, up_w, preferred_element_type=jnp.float32)
        gate_clamped = jnp.minimum(pre_gate, clamp_limit)
        up_clamped = jnp.clip(pre_up, -clamp_limit, clamp_limit)
        sigmoid_gate = jax.nn.sigmoid(sig_slope * gate_clamped)
        gated_act = gate_clamped * sigmoid_gate
        activation = ((up_clamped + 1.0) * gated_act).astype(jnp.bfloat16)
        back_act = jnp.dot(cot_in, down_w.T, preferred_element_type=jnp.float32)
        shares = jnp.sum(activation.astype(jnp.float32) * back_act, axis=1)
        slope_term = sigmoid_gate + sig_slope * gated_act * (1.0 - sigmoid_gate)
        d_gate = jnp.where(pre_gate < clamp_limit, back_act * (up_clamped + 1.0) * slope_term, 0.0).astype(jnp.bfloat16)
        d_up = jnp.where(jnp.abs(pre_up) < clamp_limit, back_act * gated_act, 0.0).astype(jnp.bfloat16)
        grad_gate = jnp.dot(rows_in.T, d_gate, preferred_element_type=jnp.float32)
        grad_up = jnp.dot(rows_in.T, d_up, preferred_element_type=jnp.float32)
        grad_down = jnp.dot(activation.T, cot_in, preferred_element_type=jnp.float32)
        gate_groups = gate_w.astype(jnp.float32).reshape(D, N_TP, group_size)
        up_groups = up_w.astype(jnp.float32).reshape(D, N_TP, group_size)
        d_gate_groups = d_gate.astype(jnp.float32).reshape(-1, N_TP, group_size)
        d_up_groups = d_up.astype(jnp.float32).reshape(-1, N_TP, group_size)
        group_parts = jnp.einsum("rnf,dnf->nrd", d_gate_groups, gate_groups, precision=highest)
        group_parts = group_parts + jnp.einsum("rnf,dnf->nrd", d_up_groups, up_groups, precision=highest)
        rounded = lax.optimization_barrier(group_parts.astype(jnp.bfloat16)).astype(jnp.float32)
        input_rows = jnp.sum(rounded, axis=0)
        return grad_gate, grad_up, grad_down, input_rows, shares

    grad_gate, grad_up, grad_down, input_rows, shares = lax.map(one_expert, (slot_table, w_gate, w_up, w_down))
    flat_slots = slot_table.reshape(-1)
    grad_assign = jnp.zeros((assign_count + 1, D), jnp.float32).at[flat_slots].add(input_rows.reshape(-1, D))
    share_assign = jnp.zeros((assign_count + 1,), jnp.float32).at[flat_slots].add(shares.reshape(-1))
    from_experts = jnp.sum(grad_assign[:assign_count].reshape(TOKENS, TOP_K, D), axis=1)
    share_grid = share_assign[:assign_count].reshape(TOKENS, TOP_K)
    mixed_grad = share_grid - weights * jnp.sum(share_grid, axis=1, keepdims=True)
    d_logits = jnp.sum(jax.nn.one_hot(routes, EXPERTS, dtype=jnp.float32) * mixed_grad[:, :, None], axis=1)
    from_router = jnp.dot(d_logits, router.astype(jnp.float32).T, precision=highest)
    grad_tokens = (from_experts + from_router).astype(jnp.bfloat16)
    grad_router = jnp.dot(tokens.astype(jnp.float32).T, d_logits, precision=highest)
    return grad_tokens, grad_router, grad_gate, grad_up, grad_down
```

```python
import jax
import jax.numpy as jnp
from jax import lax
from jax.sharding import PartitionSpec as P

clamp_limit = 7.0
sig_slope = 1.702


def split_halves(values):
    high = lax.reduce_precision(values, 8, 7)
    return high.astype(jnp.bfloat16), (values - high).astype(jnp.bfloat16)


def on_device(tokens, routes, router, w_gate, w_up, w_down, cotangent):
    f32, bf16 = jnp.float32, jnp.bfloat16
    ep_count = lax.axis_size("ep")
    tp_count = lax.axis_size("tp")
    ep_index = lax.axis_index("ep")
    tp_index = lax.axis_index("tp")
    tok_rows, model_width = tokens.shape
    top_count = routes.shape[1]
    local_experts = w_gate.shape[0]
    hidden = w_gate.shape[2]
    all_experts = ep_count * local_experts
    capacity = 3 * tok_rows * top_count // (2 * all_experts)
    slot_count = all_experts * capacity
    part = model_width // tp_count
    cores = 2
    ys = tp_count // cores
    y_index, core_index = tp_index // cores, tp_index % cores
    to_core = [(i, i // cores * cores + (i + 1) % cores) for i in range(tp_count)]

    def to_y(step):
        return [(i, (i + step * cores) % tp_count) for i in range(tp_count)]

    logits = jnp.dot(tokens, router, preferred_element_type=f32)
    experts = jnp.arange(all_experts, dtype=jnp.int32)
    hot = jnp.any(routes[:, :, None] == experts[None, None, :], axis=1)
    top = jnp.max(jnp.where(hot, logits, -jnp.inf), axis=1, keepdims=True)
    powers = jnp.where(hot, jnp.exp(jnp.minimum(logits - top, 0.0)), 0.0)
    weights = powers / jnp.sum(powers, axis=1, keepdims=True)
    hot_t = hot.T.astype(bf16)
    rows_at = jnp.arange(tok_rows, dtype=jnp.int32)
    before = (rows_at[:, None] < rows_at[None, :]).astype(bf16)
    earlier = jnp.dot(hot_t, before, preferred_element_type=f32)
    place = jnp.where(hot.T, earlier, -1.0).astype(jnp.int32)
    dispatch = place[:, None, :] == jnp.arange(capacity, dtype=jnp.int32)[None, :, None]
    slot_weight = jnp.sum(jnp.where(dispatch, weights.T[:, None, :], 0.0), axis=2).reshape(slot_count)
    dispatch = dispatch.reshape(slot_count, tok_rows).astype(bf16)
    token_cols = lax.dynamic_slice_in_dim(tokens, tp_index * part, part, 1)
    cot_cols = lax.dynamic_slice_in_dim(cotangent, tp_index * part, part, 1)
    meta_width = -(-2 * all_experts // 128) * 128
    high, low = split_halves(weights)
    meta = jnp.pad(jnp.concatenate([high, low], axis=1), ((0, 0), (0, meta_width - 2 * all_experts)))
    sent_tok = jnp.dot(dispatch, token_cols, preferred_element_type=f32).astype(bf16)
    sent_cot = (slot_weight[:, None] * jnp.dot(dispatch, cot_cols, preferred_element_type=f32)).astype(bf16)
    sent_meta = jnp.dot(dispatch, meta, preferred_element_type=f32).astype(bf16)
    sent = jnp.concatenate([sent_tok, sent_cot, sent_meta], axis=1)
    sent = sent.reshape(ep_count, local_experts * capacity, 2 * part + meta_width)
    got = lax.all_to_all(sent, "ep", 0, 0, tiled=True)
    row_count = ep_count * capacity
    width = 2 * part + meta_width
    got = got.reshape(ep_count, local_experts, capacity, width).transpose(1, 0, 2, 3)
    got = got.reshape(local_experts, row_count, width)
    slot_w = got[:, :, 2 * part :].astype(f32)
    slot_w = slot_w[:, :, :all_experts] + slot_w[:, :, all_experts : 2 * all_experts]
    mine = got[:, :, : 2 * part]

    stack = jnp.stack([mine] + [lax.ppermute(mine, "tp", to_y(s)) for s in range(1, ys)])
    other = lax.ppermute(stack, "tp", to_core)
    stacks = jnp.stack([stack, other], axis=1).reshape(ys * cores, local_experts, row_count, 2 * part)

    def piece(index):
        y_from, c_from = index // cores, index % cores
        step = lax.rem(y_index - y_from + ys, ys)
        swap = lax.rem(core_index + c_from, cores)
        return lax.dynamic_index_in_dim(stacks, step * cores + swap, 0, keepdims=False)

    pieces = [piece(i) for i in range(tp_count)]
    rows = jnp.concatenate([p[:, :, :part] for p in pieces], axis=2)
    cots = jnp.concatenate([p[:, :, part:] for p in pieces], axis=2)

    pre_gate = jnp.einsum("lrd,ldf->lrf", rows, w_gate, preferred_element_type=f32)
    pre_up = jnp.einsum("lrd,ldf->lrf", rows, w_up, preferred_element_type=f32)
    gate_clamped = jnp.minimum(pre_gate, clamp_limit)
    up_clamped = jnp.clip(pre_up, -clamp_limit, clamp_limit)
    sigmoid_gate = jax.nn.sigmoid(sig_slope * gate_clamped)
    gated_act = gate_clamped * sigmoid_gate
    activation = ((up_clamped + 1.0) * gated_act).astype(bf16)
    back_act = jnp.einsum("lrd,lfd->lrf", cots, w_down, preferred_element_type=f32)
    share = jnp.sum(activation.astype(f32) * back_act, axis=2)
    slope_term = sigmoid_gate + sig_slope * gated_act * (1.0 - sigmoid_gate)
    d_gate = jnp.where(pre_gate < clamp_limit, back_act * (up_clamped + 1.0) * slope_term, 0.0).astype(bf16)
    d_up = jnp.where(jnp.abs(pre_up) < clamp_limit, back_act * gated_act, 0.0).astype(bf16)

    own = ep_index * local_experts + jnp.arange(local_experts, dtype=jnp.int32)
    own_hot = (own[:, None, None] == experts[None, None, :]).astype(f32)
    d_logits = share[:, :, None] * (own_hot - slot_w)
    d_high, d_low = split_halves(d_logits)
    row_part = jnp.einsum("lrf,ldf->lrd", d_gate, w_gate, preferred_element_type=f32)
    row_part = row_part + jnp.einsum("lrf,ldf->lrd", d_up, w_up, preferred_element_type=f32)
    row_part = row_part + jnp.einsum("lre,de->lrd", d_high, router, preferred_element_type=f32)
    row_part = row_part + jnp.einsum("lre,de->lrd", d_low, router, preferred_element_type=f32)
    row_part = row_part.astype(bf16).reshape(local_experts, row_count, ys, cores, part)
    router_part = jnp.einsum("lre,lrd->ed", d_high, rows, preferred_element_type=f32)
    router_part = router_part + jnp.einsum("lre,lrd->ed", d_low, rows, preferred_element_type=f32)
    router_part = router_part.reshape(all_experts, ys, cores, part)

    def reduce_tp(values):
        keep = lax.dynamic_index_in_dim(values, core_index, 3 if values.ndim == 5 else 2, keepdims=False)
        give = lax.dynamic_index_in_dim(values, 1 - core_index, 3 if values.ndim == 5 else 2, keepdims=False)
        axis = keep.ndim - 2
        both = (keep.astype(f32) + lax.ppermute(give, "tp", to_core).astype(f32)).astype(values.dtype)
        total = lax.dynamic_index_in_dim(both, y_index, axis, keepdims=False).astype(f32)
        for step in range(1, ys):
            there = lax.dynamic_index_in_dim(both, lax.rem(y_index + step, ys), axis, keepdims=False)
            total = total + lax.ppermute(there, "tp", to_y(step)).astype(f32)
        return total

    input_part = reduce_tp(row_part).astype(bf16)
    router_sum = reduce_tp(router_part)
    grad_gate = jnp.einsum("lrd,lrf->ldf", rows, d_gate, preferred_element_type=f32)
    grad_up = jnp.einsum("lrd,lrf->ldf", rows, d_up, preferred_element_type=f32)
    grad_down = jnp.einsum("lrf,lrd->lfd", activation, cots, preferred_element_type=f32)

    r_high, r_low = split_halves(router_sum)
    router_rows = jnp.concatenate([r_high, r_low], axis=0)
    back = input_part.reshape(local_experts, ep_count, capacity, part).transpose(1, 0, 2, 3)
    back = back.reshape(ep_count, local_experts * capacity, part)
    back = jnp.concatenate([back, jnp.broadcast_to(router_rows[None], (ep_count,) + router_rows.shape)], axis=1)
    returned = lax.all_to_all(back, "ep", 0, 0, tiled=True)
    back_rows = returned[:, : local_experts * capacity].reshape(slot_count, part)
    grad_tokens = lax.dot_general(dispatch, back_rows, (((0,), (0,)), ((), ())), preferred_element_type=f32).astype(bf16)
    terms = returned[:, local_experts * capacity :].astype(f32).reshape(ep_count * 2, all_experts, part)
    grad_router = jnp.sum(terms, axis=0).T
    return (grad_tokens, grad_router, grad_gate, grad_up, grad_down)


def solution(mesh):
    return jax.shard_map(
        on_device,
        mesh=mesh,
        in_specs=(
            P("ep", None),
            P("ep", None),
            P(),
            P("ep", None, "tp"),
            P("ep", None, "tp"),
            P("ep", "tp", None),
            P("ep", None),
        ),
        out_specs=(
            P("ep", "tp"),
            P("tp", None),
            P("ep", None, "tp"),
            P("ep", None, "tp"),
            P("ep", "tp", None),
        ),
        check_vma=False,
    )
```

```python
import functools

import jax
import jax.numpy as jnp
from jax import lax
from jax.experimental import pallas as pl
from jax.experimental.pallas import tpu as pltpu
from jax.sharding import PartitionSpec as P

clamp_limit = 7.0
sig_slope = 1.702
cores = 2
lanes = 128


f32, bf16, i32 = jnp.float32, jnp.bfloat16, jnp.int32


def round_up(value, step):
    return -(-value // step) * step


def call(kernel, outs, args, flops, scratch=()):
    vmem = pl.BlockSpec(memory_space=pltpu.VMEM)
    moved = sum(a.size * a.dtype.itemsize for a in args) + sum(o.size * o.dtype.itemsize for o in outs)
    return pl.pallas_call(
        kernel,
        out_shape=outs,
        in_specs=[vmem] * len(args),
        out_specs=[vmem] * len(outs),
        scratch_shapes=list(scratch),
        compiler_params=pltpu.CompilerParams(vmem_limit_bytes=40 * 2**20),
        cost_estimate=pl.CostEstimate(flops=flops, bytes_accessed=moved, transcendentals=0),
    )(*args)


def shaped(shape, dtype):
    return jax.ShapeDtypeStruct(shape, dtype)


def dot(a, b, contract):
    return lax.dot_general(a, b, ((contract[:1], contract[1:]), ((), ())), preferred_element_type=f32)


def iota(shape, axis):
    return lax.broadcasted_iota(i32, shape, axis)


def pack_kernel(experts, capacity, part, tokens, routes, router, cotangent, *rest):
    dispatch, blocks, (place_at, weight_at) = rest[0], rest[1:-2], rest[-2:]
    ep_count = len(blocks)
    ep_index = lax.axis_index("ep")
    start = pl.multiple_of(lax.axis_index("tp") * part, lanes)
    rows = tokens.shape[0]
    wide = router.shape[1]
    logits = dot(tokens[...], router[...], (1, 0))
    lane = iota((rows, wide), 1)
    hot = lane == routes[:, 0:1]
    for k in range(1, routes.shape[1]):
        hot = hot | (lane == routes[:, k : k + 1])
    top = jnp.max(jnp.where(hot, logits, -jnp.inf), axis=1, keepdims=True)
    powers = jnp.where(hot, jnp.exp(jnp.where(hot, logits - top, 0.0)), 0.0)
    weights = powers / jnp.sum(powers, axis=1, keepdims=True)
    before = (iota((rows, rows), 1) < iota((rows, rows), 0)).astype(bf16)
    earlier = dot(before, jnp.where(hot, 1.0, 0.0).astype(bf16), (1, 0))
    place_at[...] = jnp.where(hot, earlier, -1.0).T
    weight_at[...] = weights.T
    high = weights.astype(bf16).astype(f32)
    meta = (high + pltpu.roll(weights - high, experts, 1)).astype(bf16)
    tok = tokens[:, pl.ds(start, part)]
    cot = cotangent[:, pl.ds(start, part)]
    slots = iota((capacity, rows), 0).astype(f32)
    for step in range(ep_count):
        expert = lax.rem(ep_index + step, ep_count)
        chosen = slots == place_at[pl.ds(expert, 1), :]
        slot_weight = jnp.sum(jnp.where(chosen, weight_at[pl.ds(expert, 1), :], 0.0), axis=1, keepdims=True)
        pick = jnp.where(chosen, 1.0, 0.0).astype(bf16)
        dispatch[expert] = pick
        block = blocks[step]
        block[:, :part] = dot(pick, tok, (1, 0)).astype(bf16)
        block[:, part : 2 * part] = (slot_weight * dot(pick, cot, (1, 0))).astype(bf16)
        block[:, 2 * part :] = dot(pick, meta, (1, 0)).astype(bf16)


def place_pieces(full, own, swapped, part):
    ys = len(own)
    y_index, core = lax.axis_index("tp") // cores, lax.axis_index("tp") % cores
    for step in range(ys):
        y_from = lax.rem(y_index - step + ys, ys)
        for pieces, c_from in ((own, core), (swapped, 1 - core)):
            at = pl.multiple_of((y_from * cores + c_from) * part, lanes)
            full[:, pl.ds(at, part)] = pieces[step][...]


def gate_kernel(ys, *refs):
    own, swapped = refs[:ys], refs[ys : 2 * ys]
    w_gate, w_up, rows, act, gate_slope, up_slope = refs[2 * ys :]
    place_pieces(rows, own, swapped, own[0].shape[1])
    hidden = w_gate.shape[1]
    tile = min(hidden, 256)
    for at in range(0, hidden, tile):
        cols = slice(at, at + tile)
        pre_gate = dot(rows[...], w_gate[:, cols], (1, 0))
        pre_up = dot(rows[...], w_up[:, cols], (1, 0))
        gate_clamped = jnp.minimum(pre_gate, clamp_limit)
        up_one = jnp.clip(pre_up, -clamp_limit, clamp_limit) + 1.0
        sig = jax.nn.sigmoid(sig_slope * gate_clamped)
        gated = gate_clamped * sig
        act[:, cols] = (up_one * gated).astype(bf16)
        slope = sig + sig_slope * gated * (1.0 - sig)
        gate_slope[:, cols] = jnp.where(pre_gate < clamp_limit, up_one * slope, 0.0)
        up_slope[:, cols] = jnp.where(jnp.abs(pre_up) < clamp_limit, gated, 0.0)


def back_kernel(ys, experts, *refs):
    own, swapped = refs[:ys], refs[ys : 2 * ys]
    act, gate_slope, up_slope, rows, meta, w_gate, w_up, w_down, router2 = refs[2 * ys : 2 * ys + 9]
    cots, d_gate, d_up = refs[2 * ys + 9 : 2 * ys + 12]
    outs = refs[2 * ys + 12 :]
    keep, give = outs[:ys], outs[ys:]
    part = own[0].shape[1]
    place_pieces(cots, own, swapped, part)
    count = cots.shape[0]
    hidden = act.shape[1]
    tile = min(hidden, 256)
    share = jnp.zeros((count, 1), f32)
    for at in range(0, hidden, tile):
        cols = slice(at, at + tile)
        back = dot(cots[...], w_down[cols, :], (1, 1))
        share = share + jnp.sum(act[:, cols].astype(f32) * back, axis=1, keepdims=True)
        d_gate[:, cols] = (back * gate_slope[:, cols]).astype(bf16)
        d_up[:, cols] = (back * up_slope[:, cols]).astype(bf16)
    wide = meta.shape[1]
    packed = meta[...].astype(f32)
    weights = packed + pltpu.roll(packed, wide - experts, 1)
    lane = iota((count, wide), 1)
    coef = jnp.where(lane == lax.axis_index("ep"), 1.0, 0.0) - weights
    d_logits = jnp.where(lane < experts, share * coef, 0.0)
    high = d_logits.astype(bf16)
    low = (d_logits - high.astype(f32)).astype(bf16)
    both = jnp.concatenate([high, low], axis=1)
    y_index, core = lax.axis_index("tp") // cores, lax.axis_index("tp") % cores
    extra = keep[0].shape[0] - count
    for step in reversed(range(ys)):
        y_to = lax.rem(y_index + step, ys)
        for out, c_to in ((give[step], 1 - core), (keep[step], core)):
            at = pl.multiple_of((y_to * cores + c_to) * part, lanes)
            value = dot(d_gate[...], w_gate[pl.ds(at, part), :], (1, 1))
            value = value + dot(d_up[...], w_up[pl.ds(at, part), :], (1, 1))
            value = value + dot(both, router2[pl.ds(at, part), :], (1, 1))
            out[:count, :] = value.astype(bf16)
            term = dot(both, rows[:, pl.ds(at, part)], (0, 0))
            out[count:, :] = (term[:extra] + term[wide : wide + extra]).astype(bf16)


def add_kernel(a, b, out):
    out[...] = (a[...].astype(f32) + b[...].astype(f32)).astype(bf16)


def return_kernel(capacity, *refs):
    parts, out = refs[:-1], refs[-1]
    ep_count = out.shape[0]
    ep_index = lax.axis_index("ep")
    count = ep_count * capacity
    total = parts[0][...].astype(f32)
    for other in parts[1:]:
        total = total + other[...].astype(f32)
    total = total.astype(bf16)
    for step in range(ep_count):
        to = lax.rem(ep_index - step + ep_count, ep_count)
        out[to, :capacity, :] = total[step * capacity : (step + 1) * capacity]
        out[to, capacity:, :] = total[count:]


def combine_kernel(experts, dispatch, back, grad_tokens, grad_router):
    ep_count, capacity = dispatch.shape[:2]
    total = dot(dispatch[0], back[0, :capacity], (0, 0))
    term = back[0, capacity:].astype(f32)
    for e in range(1, ep_count):
        total = total + dot(dispatch[e], back[e, :capacity], (0, 0))
        term = term + back[e, capacity:].astype(f32)
    grad_tokens[...] = total.astype(bf16)
    fill = jnp.zeros((lanes - term.shape[0], term.shape[1]), f32)
    grad_router[...] = jnp.concatenate([term, fill], axis=0).T[:, :experts]


def on_device(tokens, routes, router, w_gate, w_up, w_down, cotangent):
    ep_count = lax.axis_size("ep")
    tp_count = lax.axis_size("tp")
    tok_rows, width = tokens.shape
    w_gate, w_up, w_down = w_gate[0], w_up[0], w_down[0]
    hidden = w_gate.shape[1]
    experts = router.shape[1]
    capacity = 3 * tok_rows * routes.shape[1] // (2 * experts)
    part = width // tp_count
    ys = tp_count // cores
    count = ep_count * capacity
    wide = round_up(2 * experts, lanes)
    extra = round_up(experts, 16)
    to_core = [(i, i ^ 1) for i in range(tp_count)]

    def to_y(step):
        return [(i, (i + step * cores) % tp_count) for i in range(tp_count)]

    def to_ep(step):
        return [(i, (i + step) % ep_count) for i in range(ep_count)]

    router1 = jnp.pad(router, ((0, 0), (0, wide - experts)))
    router2 = jnp.concatenate([router1, router1], axis=1)
    packed = 2 * part + wide
    dispatch, *blocks = call(
        functools.partial(pack_kernel, experts, capacity, part),
        [shaped((ep_count, capacity, tok_rows), bf16)] + [shaped((capacity, packed), bf16)] * ep_count,
        (tokens, routes, router1, cotangent),
        2 * tok_rows * packed * count,
        [pltpu.VMEM((wide, tok_rows), f32)] * 2,
    )
    got = [blocks[0]] + [lax.ppermute(blocks[s], "ep", to_ep(s)) for s in range(1, ep_count)]
    tok = jnp.concatenate([g[:, :part] for g in got], axis=0)
    cot = jnp.concatenate([g[:, part : 2 * part] for g in got], axis=0)
    meta = jnp.concatenate([g[:, 2 * part :] for g in got], axis=0)

    def gather(mine):
        own = [mine] + [lax.ppermute(mine, "tp", to_y(s)) for s in range(1, ys)]
        return own, [lax.ppermute(o, "tp", to_core) for o in own]

    tok_own, tok_swapped = gather(tok)
    cot_own, cot_swapped = gather(cot)
    rows, act, gate_slope, up_slope = call(
        functools.partial(gate_kernel, ys),
        [shaped((count, width), bf16), shaped((count, hidden), bf16)] + [shaped((count, hidden), f32)] * 2,
        (*tok_own, *tok_swapped, w_gate, w_up),
        4 * count * width * hidden,
    )
    cots, d_gate, d_up, *sums = call(
        functools.partial(back_kernel, ys, experts),
        [shaped((count, width), bf16)]
        + [shaped((count, hidden), bf16)] * 2
        + [shaped((count + extra, part), bf16)] * (2 * ys),
        (*cot_own, *cot_swapped, act, gate_slope, up_slope, rows, meta, w_gate, w_up, w_down, router2),
        6 * count * width * hidden,
    )
    keep, give = sums[:ys], sums[ys:]
    pairs = [None] * ys
    for step in reversed(range(ys)):
        came = lax.ppermute(give[step], "tp", to_core)
        (pairs[step],) = call(add_kernel, [shaped(came.shape, bf16)], (keep[step], came), came.size)
    terms = [pairs[0]] + [lax.ppermute(pairs[s], "tp", to_y(s)) for s in range(1, ys)]
    (back,) = call(
        functools.partial(return_kernel, capacity),
        [shaped((ep_count, capacity + extra, part), bf16)],
        tuple(terms),
        count * part,
    )
    returned = lax.all_to_all(back, "ep", 0, 0, tiled=True)
    grad_gate = dot(rows, d_gate, (0, 0))
    grad_up = dot(rows, d_up, (0, 0))
    grad_down = dot(act, cots, (0, 0))
    grad_tokens, grad_router = call(
        functools.partial(combine_kernel, experts),
        [shaped((tok_rows, part), bf16), shaped((part, experts), f32)],
        (dispatch, returned),
        2 * tok_rows * part * count,
    )
    return (grad_tokens, grad_router, grad_gate[None], grad_up[None], grad_down[None])


def solution(mesh):
    return jax.shard_map(
        on_device,
        mesh=mesh,
        in_specs=(
            P("ep", None),
            P("ep", None),
            P(),
            P("ep", None, "tp"),
            P("ep", None, "tp"),
            P("ep", "tp", None),
            P("ep", None),
        ),
        out_specs=(
            P("ep", "tp"),
            P("tp", None),
            P("ep", None, "tp"),
            P("ep", None, "tp"),
            P("ep", "tp", None),
        ),
        check_vma=False,
    )
```

```python
import functools
import math

import jax
import jax.numpy as jnp
from jax import lax
from jax.experimental import pallas as pl
from jax.experimental.pallas import tpu as pltpu
from jax.sharding import PartitionSpec as P


clamp_limit = 7.0
sig_slope = 1.702
cores = 2
groups = 2
lanes = 128
vmem_grant = 16 * 2**20


f32, bf16, i32 = jnp.float32, jnp.bfloat16, jnp.int32


def round_up(value, step):
    return -(-value // step) * step


def call(kernel, outs, args, flops, scratch=(), in_hbm=(), aliases=None, out_in_hbm=()):
    vmem, hbm = pl.BlockSpec(memory_space=pltpu.VMEM), pl.BlockSpec(memory_space=pltpu.HBM)
    args = [pltpu.with_memory_space_constraint(a, pltpu.HBM) if i in in_hbm else a for i, a in enumerate(args)]
    moved = sum(a.size * a.dtype.itemsize for a in args) + sum(2 * math.prod(o.shape) for o in outs)
    return pl.pallas_call(
        kernel,
        out_shape=outs,
        in_specs=[hbm if i in in_hbm else vmem for i in range(len(args))],
        out_specs=[hbm if i in out_in_hbm else vmem for i in range(len(outs))],
        scratch_shapes=list(scratch),
        input_output_aliases=aliases or {},
        compiler_params=pltpu.CompilerParams(vmem_limit_bytes=vmem_grant),
        cost_estimate=pl.CostEstimate(flops=flops, bytes_accessed=moved, transcendentals=0),
    )(*args)


def shaped(shape, dtype):
    return jax.ShapeDtypeStruct(shape, dtype)


def dot(a, b, contract):
    return lax.dot_general(a, b, ((contract[:1], contract[1:]), ((), ())), preferred_element_type=f32)


def iota(shape, axis):
    return lax.broadcasted_iota(i32, shape, axis)


def power_block(count):
    return count & -count


def moved_to(index, step, ep_count, sign):
    turn, flip = step
    block = power_block(ep_count)
    turns = ep_count // block
    return lax.rem(index // block + turns + sign * turn, turns) * block + lax.bitwise_xor(lax.rem(index, block), flip)


def tp_place():
    index = lax.axis_index("tp")
    return index // cores, lax.rem(index, cores)


def pack_kernel(order, near, experts, part, *refs):
    sources, dispatch, blocks = refs[:4], refs[4], refs[5:-7]
    targets, (place_at, weight_at, sems) = refs[-7:-3], refs[-3:]
    copies = [pltpu.make_async_copy(s, t, sems.at[i]) for i, (s, t) in enumerate(zip(sources, targets))]
    for copy in copies:
        copy.start()
    for copy in copies:
        copy.wait()
    tokens, routes, router, cotangent = targets
    ep_count = len(blocks)
    ep_index, tp_index = lax.axis_index("ep"), lax.axis_index("tp")
    rows, width = tokens.shape
    capacity = dispatch.shape[1]
    logits = dot(router[...], tokens[...], (1, 1))
    expert_at = iota((experts, rows), 0)
    hot = expert_at == routes[0:1, :]
    for k in range(1, routes.shape[0]):
        hot = hot | (expert_at == routes[k : k + 1, :])
    top = jnp.max(jnp.where(hot, logits, -jnp.inf), axis=0, keepdims=True)
    powers = jnp.where(hot, jnp.exp(jnp.where(hot, logits - top, 0.0)), 0.0)
    weights = powers / jnp.sum(powers, axis=0, keepdims=True)
    before = (iota((rows, rows), 0) < iota((rows, rows), 1)).astype(bf16)
    earlier = dot(jnp.where(hot, 1.0, 0.0).astype(bf16), before, (1, 0))
    place_at[:experts, :] = jnp.where(hot, earlier, -1.0)
    weight_at[...] = jnp.zeros_like(weight_at)
    weight_at[:experts, :] = weights
    full = weight_at[...].T
    high = full.astype(bf16).astype(f32)
    meta = (high + pltpu.roll(full - high, experts, 1)).astype(bf16)
    slots = iota((capacity, rows), 0).astype(f32)
    for index, (step, block) in enumerate(zip(order, blocks)):
        expert = moved_to(ep_index, step, ep_count, 1)
        chosen = slots == place_at[pl.ds(expert, 1), :]
        slot_weight = jnp.sum(jnp.where(chosen, weight_at[pl.ds(expert, 1), :], 0.0), axis=1, keepdims=True)
        pick = jnp.where(chosen, 1.0, 0.0).astype(bf16)
        dispatch[expert] = pick
        if index == 0:
            span, start = width, 0
        elif index < near:
            span = width // cores
            start = pl.multiple_of(lax.rem(tp_index, cores) * span, lanes)
        else:
            span = part
            start = pl.multiple_of(tp_index * span, lanes)
        block[:, :span] = dot(pick, tokens[:, pl.ds(start, span)], (1, 0)).astype(bf16)
        cots = dot(pick, cotangent[:, pl.ds(start, span)], (1, 0))
        block[:, span : 2 * span] = (slot_weight * cots).astype(bf16)
        block[:, 2 * span :] = dot(pick, meta, (1, 0)).astype(bf16)


def stage_kernel(source, target, sem):
    copy = pltpu.make_async_copy(source, target, sem)
    copy.start()
    copy.wait()


def put(rows, cots, piece, first, at, span):
    count = piece.shape[0]
    cols = pl.ds(at if isinstance(at, int) else pl.multiple_of(at, lanes), span)
    rows[first : first + count, cols] = piece[:, :span]
    cots[first : first + count, cols] = piece[:, span : 2 * span]


def expert_kernel(ys, experts, group, last, *refs):
    refs = list(refs)

    def take(count):
        taken = refs[:count]
        del refs[:count]
        return taken

    sent = take(3 if group == 0 else 2 * ys + 1)
    w_gate, w_up, w_down, router = take(4)
    if group:
        before = take(2 * ys)
        take(5)
    all_rows, all_cots, all_act, all_d_gate, all_d_up = take(5)
    outs = take(2 * ys)
    terms = [] if last else take(2 * ys)
    rows, cots, sem = refs
    count, width = cots.shape
    part = width // (cores * ys)
    y_index, core = tp_place()
    mine = pl.ds(group * count, count)
    act, d_gate, d_up = [r.at[mine] for r in (all_act, all_d_gate, all_d_up)]
    if group == 0:
        own, near, swapped = sent
        half = width // cores
        put(rows, cots, own, 0, 0, width)
        put(rows, cots, near, own.shape[0], core * half, half)
        put(rows, cots, swapped, own.shape[0], (1 - core) * half, half)
        meta = jnp.concatenate([own[:, 2 * width :], near[:, 2 * half :]], axis=0)
    else:
        meta = sent[2 * ys][...]
        for step in range(ys):
            y_from = lax.rem(y_index - step + ys, ys)
            put(rows, cots, sent[step], 0, (y_from * cores + core) * part, part)
            put(rows, cots, sent[ys + step], 0, (y_from * cores + 1 - core) * part, part)
    saves = [
        pltpu.make_async_copy(rows, all_rows.at[mine], sem.at[0]),
        pltpu.make_async_copy(cots, all_cots.at[mine], sem.at[1]),
    ]
    for save in saves:
        save.start()
    hidden = act.shape[1]
    tile = min(hidden, 256)
    share = jnp.zeros((count, 1), f32)
    for at in range(0, hidden, tile):
        cols = slice(at, at + tile)
        pre_gate = dot(rows[...], w_gate[:, cols], (1, 0))
        pre_up = dot(rows[...], w_up[:, cols], (1, 0))
        back = dot(cots[...], w_down[cols, :], (1, 1))
        gate_clamped = jnp.minimum(pre_gate, clamp_limit)
        up_one = jnp.clip(pre_up, -clamp_limit, clamp_limit) + 1.0
        sig = jax.nn.sigmoid(sig_slope * gate_clamped)
        gated = gate_clamped * sig
        made = (up_one * gated).astype(bf16)
        act[:, cols] = made
        share = share + jnp.sum(made.astype(f32) * back, axis=1, keepdims=True)
        slope = sig + sig_slope * gated * (1.0 - sig)
        d_gate[:, cols] = jnp.where(pre_gate < clamp_limit, back * up_one * slope, 0.0).astype(bf16)
        d_up[:, cols] = jnp.where(jnp.abs(pre_up) < clamp_limit, back * gated, 0.0).astype(bf16)
    wide = meta.shape[1]
    packed = meta.astype(f32)
    weights = packed + pltpu.roll(packed, wide - experts, 1)
    lane = iota((count, wide), 1)
    coef = jnp.where(lane == lax.axis_index("ep"), 1.0, 0.0) - weights
    d_logits = jnp.where(lane < experts, share * coef, 0.0)
    high = d_logits.astype(bf16)
    low = (d_logits - high.astype(f32)).astype(bf16)
    both = jnp.concatenate([high, low], axis=1)
    fill = jnp.zeros((wide - experts, part), f32)
    for step in reversed(range(ys)):
        y_to = lax.rem(y_index + step, ys)
        for index, c_to in ((ys + step, 1 - core), (step, core)):
            at = pl.multiple_of((y_to * cores + c_to) * part, lanes)
            value = dot(d_gate[...], w_gate[pl.ds(at, part), :], (1, 1))
            value = value + dot(d_up[...], w_up[pl.ds(at, part), :], (1, 1))
            side = jnp.concatenate([router[:, pl.ds(at, part)].astype(f32), fill], axis=0).astype(bf16)
            value = value + dot(both, jnp.concatenate([side, side], axis=0), (1, 0))
            outs[index][:count, :] = value.astype(bf16)
            term = dot(both, rows[:, pl.ds(at, part)], (0, 0))
            term = term[:experts] + term[wide : wide + experts]
            if group:
                term = term + before[index][...]
            if last:
                outs[index][count:, :] = term.astype(bf16)
            else:
                terms[index][...] = term
    for save in saves:
        save.wait()


def add_kernel(a, b, out):
    out[...] = (a[...].astype(f32) + b[...].astype(f32)).astype(bf16)


def return_kernel(order, capacity, *refs):
    parts, out = refs[:-1], refs[-1]
    ep_count = out.shape[0]
    ep_index = lax.axis_index("ep")
    ys = len(parts) // groups
    held = ep_count // groups
    for group in range(groups):
        total = parts[group * ys][...].astype(f32)
        for other in parts[group * ys + 1 : (group + 1) * ys]:
            total = total + other[...].astype(f32)
        total = total.astype(bf16)
        for at in range(held):
            to = moved_to(ep_index, order[group * held + at], ep_count, -1)
            out[to, :capacity, :] = total[at * capacity : (at + 1) * capacity]
    for to in range(ep_count):
        out[to, capacity:, :] = total[held * capacity :]


def grads_kernel(rows, cots, act, d_gate, d_up, gate, up, down, act_t):
    @pl.when(pl.program_id(0) == 0)
    def _():
        act_t[...] = act[...].T

    rows_t = rows[...].T
    gate[...] = dot(rows_t, d_gate[...], (1, 0))
    up[...] = dot(rows_t, d_up[...], (1, 0))
    down[...] = dot(act_t[...], cots[...], (1, 0))


def weight_grads(made, width, hidden, tile):
    count = made[0].shape[0]
    tall = pl.BlockSpec((tile, hidden), lambda i: (i, 0))
    some = pl.BlockSpec((count, tile), lambda i: (0, i))
    whole = pl.BlockSpec(memory_space=pltpu.VMEM)
    made = [pltpu.with_memory_space_constraint(m, pltpu.HBM) for m in made[:2]] + list(made[2:])
    return pl.pallas_call(
        grads_kernel,
        grid=(width // tile,),
        out_shape=[shaped((width, hidden), f32)] * 2 + [shaped((hidden, width), f32)],
        in_specs=[some, some, whole, whole, whole],
        out_specs=[tall, tall, pl.BlockSpec((hidden, tile), lambda i: (0, i))],
        scratch_shapes=[pltpu.VMEM((hidden, count), bf16)],
        compiler_params=pltpu.CompilerParams(vmem_limit_bytes=vmem_grant),
        cost_estimate=pl.CostEstimate(
            flops=6 * count * width * hidden, bytes_accessed=12 * width * hidden, transcendentals=0
        ),
    )(*made)


def combine_kernel(dispatch, back, grad_tokens, grad_router):
    ep_count, capacity = dispatch.shape[:2]
    total = dot(dispatch[0], back[0, :capacity], (0, 0))
    term = back[0, capacity:].astype(f32)
    for e in range(1, ep_count):
        total = total + dot(dispatch[e], back[e, :capacity], (0, 0))
        term = term + back[e, capacity:].astype(f32)
    grad_tokens[...] = total.astype(bf16)
    grad_router[...] = term


def on_device(tokens, routes, router, w_gate, w_up, w_down, cotangent):
    ep_count = lax.axis_size("ep")
    tp_count = lax.axis_size("tp")
    tok_rows, width = tokens.shape
    w_gate, w_up, w_down = w_gate[0], w_up[0], w_down[0]
    hidden = w_gate.shape[1]
    experts = router.shape[1]
    capacity = 3 * tok_rows * routes.shape[1] // (2 * experts)
    part, half = width // tp_count, width // cores
    ys = tp_count // cores
    held = ep_count // groups
    count = held * capacity
    wide = round_up(2 * experts, lanes)
    block = power_block(ep_count)
    order = [(turn, flip) for turn in range(ep_count // block) for flip in range(block)]
    to_core = [(i, i ^ 1) for i in range(tp_count)]

    def to_y(step):
        return [(i, (i + step * cores) % tp_count) for i in range(tp_count)]

    def to_ep(step):
        turn, flip = step
        return [(i, (i // block + turn) % (ep_count // block) * block + (i % block ^ flip)) for i in range(ep_count)]

    spans = [width] + [half] * (held - 1) + [part] * (ep_count - held)
    dispatch, *blocks = call(
        functools.partial(pack_kernel, order, held, experts, part),
        [shaped((ep_count, capacity, tok_rows), bf16)] + [shaped((capacity, 2 * s + wide), bf16) for s in spans],
        (tokens, routes.T, router.T, cotangent),
        2 * tok_rows * capacity * (2 * sum(spans) + wide * ep_count),
        [
            pltpu.VMEM(tokens.shape, bf16),
            pltpu.VMEM(routes.shape[::-1], i32),
            pltpu.VMEM(router.shape[::-1], bf16),
            pltpu.VMEM(cotangent.shape, bf16),
            pltpu.VMEM((wide, tok_rows), f32),
            pltpu.VMEM((wide, tok_rows), f32),
            pltpu.SemaphoreType.DMA((4,)),
        ],
        range(4),
    )
    (w_down,) = call(stage_kernel, [shaped(w_down.shape, bf16)], (w_down,), 10**9, [pltpu.SemaphoreType.DMA], (0,))
    got = [blocks[0]]
    for at in range(1, ep_count):
        got.append(lax.ppermute(blocks[at], "ep", to_ep(order[at])))
    made, terms, sums = (), (), []
    for group in range(groups):
        last = group == groups - 1
        here = got[group * held : (group + 1) * held]
        if group == 0:
            near = jnp.concatenate(here[1:], axis=0)
            sent = (here[0], near, lax.ppermute(near, "tp", to_core))
        else:
            mine = jnp.concatenate([g[:, : 2 * part] for g in here], axis=0)
            meta = jnp.concatenate([g[:, 2 * part :] for g in here], axis=0)
            own = [mine] + [lax.ppermute(mine, "tp", to_y(s)) for s in range(1, ys)]
            swapped = [lax.ppermute(own[0], "tp", to_core)]
            swapped += [lax.ppermute(o, "tp", to_core) for o in own[1:]]
            sent = (*own, *swapped, meta)
        outs = [pltpu.HBM((groups * count, width), bf16)] * 2 + [shaped((groups * count, hidden), bf16)] * 3
        outs = outs + [shaped((count + experts if last else count, part), bf16)] * (2 * ys)
        if not last:
            outs = outs + [shaped((experts, part), f32)] * (2 * ys)
        args = (*sent, w_gate, w_up, w_down, router.T, *terms)
        at = len(args)
        got_outs = call(
            functools.partial(expert_kernel, ys, experts, group, last),
            outs,
            (*args, *made),
            10 * count * width * hidden,
            [pltpu.VMEM((count, width), bf16), pltpu.VMEM((count, width), bf16), pltpu.SemaphoreType.DMA((2,))],
            (at, at + 1) if group else (),
            {at + i: i for i in range(5)} if group else None,
            (0, 1),
        )
        made = got_outs[:5]
        terms = got_outs[5 + 2 * ys :]
        keep, give = got_outs[5 : 5 + ys], got_outs[5 + ys : 5 + 2 * ys]
        pairs = [None] * ys
        for step in reversed(range(ys)):
            came = lax.ppermute(give[step], "tp", to_core)
            (pairs[step],) = call(add_kernel, [shaped(came.shape, bf16)], (keep[step], came), came.size)
        sums += [pairs[0]] + [lax.ppermute(pairs[s], "tp", to_y(s)) for s in range(1, ys)]
    (back,) = call(
        functools.partial(return_kernel, order, capacity),
        [shaped((ep_count, capacity + experts, part), bf16)],
        tuple(sums),
        count * part,
    )
    returned = lax.all_to_all(back, "ep", 0, 0, tiled=True)
    grad_gate, grad_up, grad_down = weight_grads(made, width, hidden, min(256, width))
    grad_tokens, grad_router = call(
        combine_kernel,
        [shaped((tok_rows, part), bf16), shaped((experts, part), f32)],
        (dispatch, returned),
        2 * tok_rows * part * capacity * ep_count,
    )
    return (grad_tokens, grad_router.T, grad_gate[None], grad_up[None], grad_down[None])


def solution(mesh):
    return jax.shard_map(
        on_device,
        mesh=mesh,
        in_specs=(
            P("ep", None),
            P("ep", None),
            P(),
            P("ep", None, "tp"),
            P("ep", None, "tp"),
            P("ep", "tp", None),
            P("ep", None),
        ),
        out_specs=(
            P("ep", "tp"),
            P("tp", None),
            P("ep", None, "tp"),
            P("ep", None, "tp"),
            P("ep", "tp", None),
        ),
        check_vma=False,
    )
```

```python
import functools
import math

import jax
import jax.numpy as jnp
from jax import lax
from jax.experimental import pallas as pl
from jax.experimental.pallas import tpu as pltpu
from jax.sharding import PartitionSpec as P


clamp_limit = 7.0
sig_slope = 1.702
cores = 2
groups = 2
lanes = 128
vmem_grant = 16 * 2**20


f32, bf16, i32 = jnp.float32, jnp.bfloat16, jnp.int32


def round_up(value, step):
    return -(-value // step) * step


def call(kernel, outs, args, flops, scratch=(), in_hbm=(), aliases=None, out_in_hbm=()):
    vmem, hbm = pl.BlockSpec(memory_space=pltpu.VMEM), pl.BlockSpec(memory_space=pltpu.HBM)
    args = [pltpu.with_memory_space_constraint(a, pltpu.HBM) if i in in_hbm else a for i, a in enumerate(args)]
    moved = sum(a.size * a.dtype.itemsize for a in args) + sum(2 * math.prod(o.shape) for o in outs)
    return pl.pallas_call(
        kernel,
        out_shape=outs,
        in_specs=[hbm if i in in_hbm else vmem for i in range(len(args))],
        out_specs=[hbm if i in out_in_hbm else vmem for i in range(len(outs))],
        scratch_shapes=list(scratch),
        input_output_aliases=aliases or {},
        compiler_params=pltpu.CompilerParams(vmem_limit_bytes=vmem_grant),
        cost_estimate=pl.CostEstimate(flops=flops, bytes_accessed=moved, transcendentals=0),
    )(*args)


def shaped(shape, dtype):
    return jax.ShapeDtypeStruct(shape, dtype)


def dot(a, b, contract):
    return lax.dot_general(a, b, ((contract[:1], contract[1:]), ((), ())), preferred_element_type=f32)


def iota(shape, axis):
    return lax.broadcasted_iota(i32, shape, axis)


def power_block(count):
    return count & -count


def moved_to(index, step, ep_count, sign):
    turn, flip = step
    block = power_block(ep_count)
    turns = ep_count // block
    return lax.rem(index // block + turns + sign * turn, turns) * block + lax.bitwise_xor(lax.rem(index, block), flip)


def tp_place():
    index = lax.axis_index("tp")
    return index // cores, lax.rem(index, cores)


def pack_kernel(order, near, experts, part, *refs):
    sources, dispatch, blocks = refs[:4], refs[4], refs[5:-7]
    targets, (place_at, weight_at, sems) = refs[-7:-3], refs[-3:]
    copies = [pltpu.make_async_copy(s, t, sems.at[i]) for i, (s, t) in enumerate(zip(sources, targets))]
    for copy in copies:
        copy.start()
    for copy in copies[:-1]:
        copy.wait()
    tokens, routes, router, cotangent = targets
    ep_count = len(blocks)
    ep_index, tp_index = lax.axis_index("ep"), lax.axis_index("tp")
    rows, width = tokens.shape
    capacity = dispatch.shape[1]
    logits = dot(router[...], tokens[...], (1, 1))
    expert_at = iota((experts, rows), 0)
    hot = expert_at == routes[0:1, :]
    for k in range(1, routes.shape[0]):
        hot = hot | (expert_at == routes[k : k + 1, :])
    top = jnp.max(jnp.where(hot, logits, -jnp.inf), axis=0, keepdims=True)
    powers = jnp.where(hot, jnp.exp(jnp.where(hot, logits - top, 0.0)), 0.0)
    weights = powers / jnp.sum(powers, axis=0, keepdims=True)
    before = (iota((rows, rows), 0) < iota((rows, rows), 1)).astype(bf16)
    earlier = dot(jnp.where(hot, 1.0, 0.0).astype(bf16), before, (1, 0))
    place_at[:experts, :] = jnp.where(hot, earlier, -1.0)
    weight_at[...] = jnp.zeros_like(weight_at)
    weight_at[:experts, :] = weights
    full = weight_at[...].T
    high = full.astype(bf16).astype(f32)
    meta = (high + pltpu.roll(full - high, experts, 1)).astype(bf16)
    low = weights - weights.astype(bf16).astype(f32)
    both_t = jnp.concatenate([weights.astype(bf16).astype(f32), low], axis=0).astype(bf16)
    slots = iota((lanes, rows), 0).astype(f32)
    copies[-1].wait()
    for index, (step, block) in enumerate(zip(order, blocks)):
        expert = moved_to(ep_index, step, ep_count, 1)
        chosen = slots == place_at[pl.ds(expert, 1), :]
        slot_weight = jnp.sum(jnp.where(chosen, weight_at[pl.ds(expert, 1), :], 0.0), axis=1, keepdims=True)
        all_pick = jnp.where(chosen, 1.0, 0.0).astype(bf16)
        pick, slot_weight = all_pick[:capacity], slot_weight[:capacity]
        dispatch[expert] = pick
        if index == 0:
            span, start = width, 0
        elif index < near:
            span = width // cores
            start = pl.multiple_of(lax.rem(tp_index, cores) * span, lanes)
        else:
            span = part
            start = pl.multiple_of(tp_index * span, lanes)
        toks = dot(pick, tokens[:, pl.ds(start, span)], (1, 0)).astype(bf16)
        cots = (slot_weight * dot(pick, cotangent[:, pl.ds(start, span)], (1, 0))).astype(bf16)
        if index < near:
            block[:, :span] = toks
            block[:, span : 2 * span] = cots
            block[:, 2 * span :] = dot(pick, meta, (1, 0)).astype(bf16)
            continue
        tall = span // lanes
        for at in range(tall):
            cols = slice(at * lanes, (at + 1) * lanes)
            block[at * capacity : (at + 1) * capacity, :] = toks[:, cols]
            block[(tall + at) * capacity : (tall + at + 1) * capacity, :] = cots[:, cols]
        block[2 * tall * capacity :, :] = dot(both_t, all_pick, (1, 1)).astype(bf16)


def stage_kernel(source, target, sem):
    copy = pltpu.make_async_copy(source, target, sem)
    copy.start()
    copy.wait()


def put(rows, cots, piece, first, at, span):
    count = piece.shape[0]
    cols = pl.ds(at if isinstance(at, int) else pl.multiple_of(at, lanes), span)
    rows[first : first + count, cols] = piece[:, :span]
    cots[first : first + count, cols] = piece[:, span : 2 * span]


def put_stacked(rows, cots, piece, blocks, at, span):
    tall = span // lanes
    high = piece.shape[0] // (2 * tall * blocks)
    for block in range(blocks):
        to = slice(block * high, (block + 1) * high)
        for col in range(tall):
            cols = pl.ds(pl.multiple_of(at + col * lanes, lanes), lanes)
            first = (2 * tall * block + col) * high
            rows[to, cols] = piece[first : first + high, :]
            first = first + tall * high
            cots[to, cols] = piece[first : first + high, :]


def expert_kernel(ys, experts, group, last, *refs):
    refs = list(refs)

    def take(count):
        taken = refs[:count]
        del refs[:count]
        return taken

    sent = take(3 if group == 0 else 2 * ys + 1)
    w_gate, w_up, w_down, router = take(4)
    if group:
        before = take(2 * ys)
        take(5)
    all_rows, all_cots, all_act, all_d_gate, all_d_up = take(5)
    outs = take(2 * ys)
    terms = [] if last else take(2 * ys)
    rows, cots, sem = refs
    count, width = cots.shape
    part = width // (cores * ys)
    y_index, core = tp_place()
    mine = pl.ds(group * count, count)
    act, d_gate, d_up = [r.at[mine] for r in (all_act, all_d_gate, all_d_up)]
    if group == 0:
        own, near, swapped = sent
        half = width // cores
        put(rows, cots, own, 0, 0, width)
        put(rows, cots, near, own.shape[0], core * half, half)
        put(rows, cots, swapped, own.shape[0], (1 - core) * half, half)
        packed = jnp.concatenate([own[:, 2 * width :], near[:, 2 * half :]], axis=0).astype(f32)
        weights = packed + pltpu.roll(packed, packed.shape[1] - experts, 1)
    else:
        packed = sent[2 * ys][...].astype(f32)
        blocks = packed.shape[0] // (2 * experts)
        for step in range(ys):
            y_from = lax.rem(y_index - step + ys, ys)
            put_stacked(rows, cots, sent[step], blocks, (y_from * cores + core) * part, part)
            put_stacked(rows, cots, sent[ys + step], blocks, (y_from * cores + 1 - core) * part, part)
        fill = jnp.zeros((lanes - experts, lanes), f32)
        weights = []
        for block in range(blocks):
            high = packed[2 * experts * block : 2 * experts * block + experts]
            low = packed[2 * experts * block + experts : 2 * experts * (block + 1)]
            weights.append(jnp.concatenate([high + low, fill], axis=0).T[: count // blocks])
        weights = jnp.concatenate(weights, axis=0)
    saves = [
        pltpu.make_async_copy(rows, all_rows.at[mine], sem.at[0]),
        pltpu.make_async_copy(cots, all_cots.at[mine], sem.at[1]),
    ]
    for save in saves:
        save.start()
    hidden = act.shape[1]
    tile = min(hidden, 256)
    share = jnp.zeros((count, 1), f32)
    for at in range(0, hidden, tile):
        cols = slice(at, at + tile)
        pre_gate = dot(rows[...], w_gate[:, cols], (1, 0))
        pre_up = dot(rows[...], w_up[:, cols], (1, 0))
        back = dot(cots[...], w_down[cols, :], (1, 1))
        gate_clamped = jnp.minimum(pre_gate, clamp_limit)
        up_one = jnp.clip(pre_up, -clamp_limit, clamp_limit) + 1.0
        sig = jax.nn.sigmoid(sig_slope * gate_clamped)
        gated = gate_clamped * sig
        made = (up_one * gated).astype(bf16)
        act[:, cols] = made
        share = share + jnp.sum(made.astype(f32) * back, axis=1, keepdims=True)
        slope = sig + sig_slope * gated * (1.0 - sig)
        d_gate[:, cols] = jnp.where(pre_gate < clamp_limit, back * up_one * slope, 0.0).astype(bf16)
        d_up[:, cols] = jnp.where(jnp.abs(pre_up) < clamp_limit, back * gated, 0.0).astype(bf16)
    wide = weights.shape[1]
    lane = iota((count, wide), 1)
    coef = jnp.where(lane == lax.axis_index("ep"), 1.0, 0.0) - weights
    d_logits = jnp.where(lane < experts, share * coef, 0.0)
    high = d_logits.astype(bf16)
    low = (d_logits - high.astype(f32)).astype(bf16)
    both = jnp.concatenate([high, low], axis=1)
    fill = jnp.zeros((wide - experts, part), f32)
    for step in reversed(range(ys)):
        y_to = lax.rem(y_index + step, ys)
        for index, c_to in ((ys + step, 1 - core), (step, core)):
            at = pl.multiple_of((y_to * cores + c_to) * part, lanes)
            value = dot(d_gate[...], w_gate[pl.ds(at, part), :], (1, 1))
            value = value + dot(d_up[...], w_up[pl.ds(at, part), :], (1, 1))
            side = jnp.concatenate([router[:, pl.ds(at, part)].astype(f32), fill], axis=0).astype(bf16)
            value = value + dot(both, jnp.concatenate([side, side], axis=0), (1, 0))
            outs[index][:count, :] = value.astype(bf16)
            term = dot(both, rows[:, pl.ds(at, part)], (0, 0))
            term = term[:experts] + term[wide : wide + experts]
            if group:
                term = term + before[index][...]
            if last:
                outs[index][count:, :] = term.astype(bf16)
            else:
                terms[index][...] = term
    for save in saves:
        save.wait()


def add_kernel(a, b, out):
    out[...] = (a[...].astype(f32) + b[...].astype(f32)).astype(bf16)


def return_kernel(order, capacity, *refs):
    parts, out = refs[:-1], refs[-1]
    ep_count = out.shape[0]
    ep_index = lax.axis_index("ep")
    ys = len(parts) // groups
    held = ep_count // groups
    for group in range(groups):
        total = parts[group * ys][...].astype(f32)
        for other in parts[group * ys + 1 : (group + 1) * ys]:
            total = total + other[...].astype(f32)
        total = total.astype(bf16)
        for at in range(held):
            to = moved_to(ep_index, order[group * held + at], ep_count, -1)
            out[to, :capacity, :] = total[at * capacity : (at + 1) * capacity]
    for to in range(ep_count):
        out[to, capacity:, :] = total[held * capacity :]


def tall_kernel(rows, d_gate, d_up, gate, up):
    gate[...] = dot(rows[...], d_gate[...], (0, 0))
    up[...] = dot(rows[...], d_up[...], (0, 0))


def flat_kernel(cots, act, down):
    down[...] = dot(act[...], cots[...], (0, 0))


def weight_grads(kernel, spread, held, out_shape, out_spec, tile):
    count, width = spread.shape
    return pl.pallas_call(
        kernel,
        grid=(width // tile,),
        out_shape=out_shape,
        in_specs=[pl.BlockSpec((count, tile), lambda i: (0, i))] + [pl.BlockSpec(memory_space=pltpu.VMEM)] * len(held),
        out_specs=out_spec,
        compiler_params=pltpu.CompilerParams(vmem_limit_bytes=vmem_grant),
        cost_estimate=pl.CostEstimate(
            flops=2 * count * sum(math.prod(o.shape) for o in out_shape),
            bytes_accessed=4 * sum(math.prod(o.shape) for o in out_shape),
            transcendentals=0,
        ),
    )(pltpu.with_memory_space_constraint(spread, pltpu.HBM), *held)


def combine_kernel(dispatch, back, grad_tokens, grad_router):
    ep_count, capacity = dispatch.shape[:2]
    total = dot(dispatch[0], back[0, :capacity], (0, 0))
    term = back[0, capacity:].astype(f32)
    for e in range(1, ep_count):
        total = total + dot(dispatch[e], back[e, :capacity], (0, 0))
        term = term + back[e, capacity:].astype(f32)
    grad_tokens[...] = total.astype(bf16)
    grad_router[...] = term


def on_device(tokens, routes, router, w_gate, w_up, w_down, cotangent):
    ep_count = lax.axis_size("ep")
    tp_count = lax.axis_size("tp")
    tok_rows, width = tokens.shape
    w_gate, w_up, w_down = w_gate[0], w_up[0], w_down[0]
    hidden = w_gate.shape[1]
    experts = router.shape[1]
    capacity = 3 * tok_rows * routes.shape[1] // (2 * experts)
    part, half = width // tp_count, width // cores
    ys = tp_count // cores
    held = ep_count // groups
    count = held * capacity
    wide = round_up(2 * experts, lanes)
    block = power_block(ep_count)
    order = [(turn, flip) for turn in range(ep_count // block) for flip in range(block)]
    to_core = [(i, i ^ 1) for i in range(tp_count)]

    def to_y(step):
        return [(i, (i + step * cores) % tp_count) for i in range(tp_count)]

    def to_ep(step):
        turn, flip = step
        return [(i, (i // block + turn) % (ep_count // block) * block + (i % block ^ flip)) for i in range(ep_count)]

    shapes = [(capacity, 2 * width + wide)] + [(capacity, 2 * half + wide)] * (held - 1)
    shapes += [(2 * part // lanes * capacity + 2 * experts, lanes)] * (ep_count - held)
    dispatch, *blocks = call(
        functools.partial(pack_kernel, order, held, experts, part),
        [shaped((ep_count, capacity, tok_rows), bf16)] + [shaped(s, bf16) for s in shapes],
        (tokens, routes.T, router.T, cotangent),
        2 * tok_rows * sum(math.prod(s) for s in shapes),
        [
            pltpu.VMEM(tokens.shape, bf16),
            pltpu.VMEM(routes.shape[::-1], i32),
            pltpu.VMEM(router.shape[::-1], bf16),
            pltpu.VMEM(cotangent.shape, bf16),
            pltpu.VMEM((wide, tok_rows), f32),
            pltpu.VMEM((wide, tok_rows), f32),
            pltpu.SemaphoreType.DMA((4,)),
        ],
        range(4),
    )
    (w_down,) = call(stage_kernel, [shaped(w_down.shape, bf16)], (w_down,), 10**9, [pltpu.SemaphoreType.DMA], (0,))
    got = [blocks[0]]
    for at in range(1, ep_count):
        got.append(lax.ppermute(blocks[at], "ep", to_ep(order[at])))
    made, terms, sums = (), (), []
    for group in range(groups):
        last = group == groups - 1
        here = got[group * held : (group + 1) * held]
        if group == 0:
            near = jnp.concatenate(here[1:], axis=0)
            sent = (here[0], near, lax.ppermute(near, "tp", to_core))
        else:
            mine = jnp.concatenate([g[: -2 * experts] for g in here], axis=0)
            meta = jnp.concatenate([g[-2 * experts :] for g in here], axis=0)
            own = [mine] + [lax.ppermute(mine, "tp", to_y(s)) for s in range(1, ys)]
            swapped = [lax.ppermute(own[0], "tp", to_core)]
            swapped += [lax.ppermute(o, "tp", to_core) for o in own[1:]]
            sent = (*own, *swapped, meta)
        outs = [pltpu.HBM((groups * count, width), bf16)] * 2 + [shaped((groups * count, hidden), bf16)] * 3
        outs = outs + [shaped((count + experts if last else count, part), bf16)] * (2 * ys)
        if not last:
            outs = outs + [shaped((experts, part), f32)] * (2 * ys)
        args = (*sent, w_gate, w_up, w_down, router.T, *terms)
        at = len(args)
        got_outs = call(
            functools.partial(expert_kernel, ys, experts, group, last),
            outs,
            (*args, *made),
            10 * count * width * hidden,
            [pltpu.VMEM((count, width), bf16), pltpu.VMEM((count, width), bf16), pltpu.SemaphoreType.DMA((2,))],
            (at, at + 1) if group else (),
            {at + i: i for i in range(5)} if group else None,
            (0, 1),
        )
        made = got_outs[:5]
        terms = got_outs[5 + 2 * ys :]
        keep, give = got_outs[5 : 5 + ys], got_outs[5 + ys : 5 + 2 * ys]
        pairs = [None] * ys
        for step in reversed(range(ys)):
            came = lax.ppermute(give[step], "tp", to_core)
            (pairs[step],) = call(add_kernel, [shaped(came.shape, bf16)], (keep[step], came), came.size)
        sums += [pairs[0]] + [lax.ppermute(pairs[s], "tp", to_y(s)) for s in range(1, ys)]
    (back,) = call(
        functools.partial(return_kernel, order, capacity),
        [shaped((ep_count, capacity + experts, part), bf16)],
        tuple(sums),
        count * part,
    )
    returned = lax.all_to_all(back, "ep", 0, 0, tiled=True)
    rows, cots, act, d_gate, d_up = made
    tile = min(512, width)
    (grad_down,) = weight_grads(
        flat_kernel, cots, (act,), [shaped((hidden, width), f32)],
        [pl.BlockSpec((hidden, tile), lambda i: (0, i))], tile,
    )
    grad_gate, grad_up = weight_grads(
        tall_kernel, rows, (d_gate, d_up), [shaped((width, hidden), f32)] * 2,
        [pl.BlockSpec((tile, hidden), lambda i: (i, 0))] * 2, tile,
    )
    grad_tokens, grad_router = call(
        combine_kernel,
        [shaped((tok_rows, part), bf16), shaped((experts, part), f32)],
        (dispatch, returned),
        2 * tok_rows * part * capacity * ep_count,
    )
    return (grad_tokens, grad_router.T, grad_gate[None], grad_up[None], grad_down[None])


def solution(mesh):
    return jax.shard_map(
        on_device,
        mesh=mesh,
        in_specs=(
            P("ep", None),
            P("ep", None),
            P(),
            P("ep", None, "tp"),
            P("ep", None, "tp"),
            P("ep", "tp", None),
            P("ep", None),
        ),
        out_specs=(
            P("ep", "tp"),
            P("tp", None),
            P("ep", None, "tp"),
            P("ep", None, "tp"),
            P("ep", "tp", None),
        ),
        check_vma=False,
    )
```

```python
import functools
import math

import jax
import jax.numpy as jnp
from jax import lax
from jax.experimental import pallas as pl
from jax.experimental.pallas import tpu as pltpu
from jax.sharding import PartitionSpec as P


clamp_limit = 7.0
sig_slope = 1.702
cores = 2
groups = 2
lanes = 128
vmem_grant = 16 * 2**20


f32, bf16, i32 = jnp.float32, jnp.bfloat16, jnp.int32


def round_up(value, step):
    return -(-value // step) * step


def call(kernel, outs, args, flops, scratch=(), in_hbm=(), aliases=None, out_in_hbm=()):
    vmem, hbm = pl.BlockSpec(memory_space=pltpu.VMEM), pl.BlockSpec(memory_space=pltpu.HBM)
    args = [pltpu.with_memory_space_constraint(a, pltpu.HBM) if i in in_hbm else a for i, a in enumerate(args)]
    moved = sum(a.size * a.dtype.itemsize for a in args) + sum(2 * math.prod(o.shape) for o in outs)
    return pl.pallas_call(
        kernel,
        out_shape=outs,
        in_specs=[hbm if i in in_hbm else vmem for i in range(len(args))],
        out_specs=[hbm if i in out_in_hbm else vmem for i in range(len(outs))],
        scratch_shapes=list(scratch),
        input_output_aliases=aliases or {},
        compiler_params=pltpu.CompilerParams(vmem_limit_bytes=vmem_grant),
        cost_estimate=pl.CostEstimate(flops=flops, bytes_accessed=moved, transcendentals=0),
    )(*args)


def shaped(shape, dtype):
    return jax.ShapeDtypeStruct(shape, dtype)


def dot(a, b, contract):
    return lax.dot_general(a, b, ((contract[:1], contract[1:]), ((), ())), preferred_element_type=f32)


def iota(shape, axis):
    return lax.broadcasted_iota(i32, shape, axis)


def power_block(count):
    return count & -count


def moved_to(index, step, ep_count, sign):
    turn, flip = step
    block = power_block(ep_count)
    turns = ep_count // block
    return lax.rem(index // block + turns + sign * turn, turns) * block + lax.bitwise_xor(lax.rem(index, block), flip)


def tp_place():
    index = lax.axis_index("tp")
    return index // cores, lax.rem(index, cores)


def pack_kernel(order, near, experts, part, *refs):
    sources, dispatch, own_weight, blocks = refs[:4], refs[4], refs[5], refs[8:-5]
    targets = (refs[6], *refs[-5:-3], refs[7])
    place_at, weight_at, sems = refs[-3:]
    copies = [pltpu.make_async_copy(s, t, sems.at[i]) for i, (s, t) in enumerate(zip(sources, targets))]
    for copy in copies:
        copy.start()
    for copy in copies[:-1]:
        copy.wait()
    tokens, routes, router, cotangent = targets
    ep_count = len(blocks)
    ep_index, tp_index = lax.axis_index("ep"), lax.axis_index("tp")
    rows, width = tokens.shape
    capacity = dispatch.shape[1]
    logits = dot(router[...], tokens[...], (1, 1))
    expert_at = iota((experts, rows), 0)
    hot = expert_at == routes[0:1, :]
    for k in range(1, routes.shape[0]):
        hot = hot | (expert_at == routes[k : k + 1, :])
    top = jnp.max(jnp.where(hot, logits, -jnp.inf), axis=0, keepdims=True)
    powers = jnp.where(hot, jnp.exp(jnp.where(hot, logits - top, 0.0)), 0.0)
    weights = powers / jnp.sum(powers, axis=0, keepdims=True)
    before = (iota((rows, rows), 0) < iota((rows, rows), 1)).astype(bf16)
    earlier = dot(jnp.where(hot, 1.0, 0.0).astype(bf16), before, (1, 0))
    place_at[:experts, :] = jnp.where(hot, earlier, -1.0)
    weight_at[...] = jnp.zeros_like(weight_at)
    weight_at[:experts, :] = weights
    full = weight_at[...].T
    high = full.astype(bf16).astype(f32)
    meta = (high + pltpu.roll(full - high, experts, 1)).astype(bf16)
    low = weights - weights.astype(bf16).astype(f32)
    both_t = jnp.concatenate([weights.astype(bf16).astype(f32), low], axis=0).astype(bf16)
    slots = iota((lanes, rows), 0).astype(f32)
    copies[-1].wait()
    for index, (step, block) in enumerate(zip(order, blocks)):
        expert = moved_to(ep_index, step, ep_count, 1)
        chosen = slots == place_at[pl.ds(expert, 1), :]
        slot_weight = jnp.sum(jnp.where(chosen, weight_at[pl.ds(expert, 1), :], 0.0), axis=1, keepdims=True)
        all_pick = jnp.where(chosen, 1.0, 0.0).astype(bf16)
        pick, slot_weight = all_pick[:capacity], slot_weight[:capacity]
        dispatch[expert] = pick
        if index == 0:
            own_weight[...] = jnp.broadcast_to(slot_weight, own_weight.shape)
            block[...] = dot(pick, meta, (1, 0)).astype(bf16)
            continue
        if index < near:
            span = width // cores
            start = pl.multiple_of(lax.rem(tp_index, cores) * span, lanes)
        else:
            span = part
            start = pl.multiple_of(tp_index * span, lanes)
        toks = dot(pick, tokens[:, pl.ds(start, span)], (1, 0)).astype(bf16)
        cots = (slot_weight * dot(pick, cotangent[:, pl.ds(start, span)], (1, 0))).astype(bf16)
        if index < near:
            block[:, :span] = toks
            block[:, span : 2 * span] = cots
            block[:, 2 * span :] = dot(pick, meta, (1, 0)).astype(bf16)
            continue
        tall = span // lanes
        for at in range(tall):
            cols = slice(at * lanes, (at + 1) * lanes)
            block[at * capacity : (at + 1) * capacity, :] = toks[:, cols]
            block[(tall + at) * capacity : (tall + at + 1) * capacity, :] = cots[:, cols]
        block[2 * tall * capacity :, :] = dot(both_t, all_pick, (1, 1)).astype(bf16)


def stage_kernel(source, dispatch, own_weight, tokens, cotangent, target, picks, own, sem):
    copy = pltpu.make_async_copy(source, target, sem)
    copy.start()
    parts = [dispatch[e].astype(f32) for e in range(dispatch.shape[0])]
    picks[...] = jnp.concatenate(parts, axis=0).T.astype(bf16)
    width = tokens.shape[1]
    pick = dispatch[lax.axis_index("ep")]
    own[:, :width] = dot(pick, tokens[...], (1, 0)).astype(bf16)
    own[:, width:] = (own_weight[:, :1] * dot(pick, cotangent[...], (1, 0))).astype(bf16)
    copy.wait()


def put(rows, cots, piece, first, at, span):
    count = piece.shape[0]
    cols = pl.ds(at if isinstance(at, int) else pl.multiple_of(at, lanes), span)
    rows[first : first + count, cols] = piece[:, :span]
    cots[first : first + count, cols] = piece[:, span : 2 * span]


def put_stacked(rows, cots, piece, blocks, at, span):
    tall = span // lanes
    high = piece.shape[0] // (2 * tall * blocks)
    for block in range(blocks):
        to = slice(block * high, (block + 1) * high)
        for col in range(tall):
            cols = pl.ds(pl.multiple_of(at + col * lanes, lanes), lanes)
            first = (2 * tall * block + col) * high
            rows[to, cols] = piece[first : first + high, :]
            first = first + tall * high
            cots[to, cols] = piece[first : first + high, :]


def expert_kernel(ys, experts, group, last, *refs):
    refs = list(refs)

    def take(count):
        taken = refs[:count]
        del refs[:count]
        return taken

    sent = take(4 if group == 0 else 2 * ys + 1)
    w_gate, w_up, w_down, router = take(4)
    if group:
        before = take(2 * ys)
        take(5)
    all_rows, all_cots, all_act, all_d_gate, all_d_up = take(5)
    outs = take(2 * ys)
    terms = [] if last else take(2 * ys)
    rows, cots, sem = refs
    count, width = cots.shape
    part = width // (cores * ys)
    y_index, core = tp_place()
    mine = pl.ds(group * count, count)
    act, d_gate, d_up = [r.at[mine] for r in (all_act, all_d_gate, all_d_up)]
    if group == 0:
        own, own_meta, near, swapped = sent
        half = width // cores
        put(rows, cots, own, 0, 0, width)
        put(rows, cots, near, own.shape[0], core * half, half)
        put(rows, cots, swapped, own.shape[0], (1 - core) * half, half)
        packed = jnp.concatenate([own_meta[...], near[:, 2 * half :]], axis=0).astype(f32)
        weights = packed + pltpu.roll(packed, packed.shape[1] - experts, 1)
    else:
        packed = sent[2 * ys][...].astype(f32)
        blocks = packed.shape[0] // (2 * experts)
        for step in range(ys):
            y_from = lax.rem(y_index - step + ys, ys)
            put_stacked(rows, cots, sent[step], blocks, (y_from * cores + core) * part, part)
            put_stacked(rows, cots, sent[ys + step], blocks, (y_from * cores + 1 - core) * part, part)
        fill = jnp.zeros((lanes - experts, lanes), f32)
        weights = []
        for block in range(blocks):
            high = packed[2 * experts * block : 2 * experts * block + experts]
            low = packed[2 * experts * block + experts : 2 * experts * (block + 1)]
            weights.append(jnp.concatenate([high + low, fill], axis=0).T[: count // blocks])
        weights = jnp.concatenate(weights, axis=0)
    saves = [
        pltpu.make_async_copy(rows, all_rows.at[mine], sem.at[0]),
        pltpu.make_async_copy(cots, all_cots.at[mine], sem.at[1]),
    ]
    for save in saves:
        save.start()
    hidden = act.shape[1]
    tile = min(hidden, 256)
    share = jnp.zeros((count, 1), f32)
    for at in range(0, hidden, tile):
        cols = slice(at, at + tile)
        pre_gate = dot(rows[...], w_gate[:, cols], (1, 0))
        pre_up = dot(rows[...], w_up[:, cols], (1, 0))
        back = dot(cots[...], w_down[cols, :], (1, 1))
        gate_clamped = jnp.minimum(pre_gate, clamp_limit)
        up_one = jnp.clip(pre_up, -clamp_limit, clamp_limit) + 1.0
        sig = jax.nn.sigmoid(sig_slope * gate_clamped)
        gated = gate_clamped * sig
        made = (up_one * gated).astype(bf16)
        act[:, cols] = made
        share = share + jnp.sum(made.astype(f32) * back, axis=1, keepdims=True)
        slope = sig + sig_slope * gated * (1.0 - sig)
        d_gate[:, cols] = jnp.where(pre_gate < clamp_limit, back * up_one * slope, 0.0).astype(bf16)
        d_up[:, cols] = jnp.where(jnp.abs(pre_up) < clamp_limit, back * gated, 0.0).astype(bf16)
    wide = weights.shape[1]
    lane = iota((count, wide), 1)
    coef = jnp.where(lane == lax.axis_index("ep"), 1.0, 0.0) - weights
    d_logits = jnp.where(lane < experts, share * coef, 0.0)
    high = d_logits.astype(bf16)
    low = (d_logits - high.astype(f32)).astype(bf16)
    both = jnp.concatenate([high, low], axis=1)
    fill = jnp.zeros((wide - experts, part), f32)
    for step in reversed(range(ys)):
        y_to = lax.rem(y_index + step, ys)
        for index, c_to in ((ys + step, 1 - core), (step, core)):
            at = pl.multiple_of((y_to * cores + c_to) * part, lanes)
            value = dot(d_gate[...], w_gate[pl.ds(at, part), :], (1, 1))
            value = value + dot(d_up[...], w_up[pl.ds(at, part), :], (1, 1))
            side = jnp.concatenate([router[:, pl.ds(at, part)].astype(f32), fill], axis=0).astype(bf16)
            value = value + dot(both, jnp.concatenate([side, side], axis=0), (1, 0))
            outs[index][:count, :] = value.astype(bf16)
            term = dot(both, rows[:, pl.ds(at, part)], (0, 0))
            term = term[:experts] + term[wide : wide + experts]
            if group:
                term = term + before[index][...]
            if last:
                outs[index][count:, :] = term.astype(bf16)
            else:
                terms[index][...] = term
    for save in saves:
        save.wait()


def add_kernel(a, b, out):
    out[...] = (a[...].astype(f32) + b[...].astype(f32)).astype(bf16)


def return_kernel(order, capacity, *refs):
    parts, out = refs[:-1], refs[-1]
    ep_count = out.shape[0]
    ep_index = lax.axis_index("ep")
    ys = len(parts) // groups
    held = ep_count // groups
    for group in range(groups):
        total = parts[group * ys][...].astype(f32)
        for other in parts[group * ys + 1 : (group + 1) * ys]:
            total = total + other[...].astype(f32)
        total = total.astype(bf16)
        for at in range(held):
            to = moved_to(ep_index, order[group * held + at], ep_count, -1)
            out[to, :capacity, :] = total[at * capacity : (at + 1) * capacity]
    for to in range(ep_count):
        out[to, capacity:, :] = total[held * capacity :]


def tall_kernel(rows, d_gate, d_up, gate, up):
    gate[...] = dot(rows[...], d_gate[...], (0, 0))
    up[...] = dot(rows[...], d_up[...], (0, 0))


def flat_kernel(cots, act, down):
    down[...] = dot(act[...], cots[...], (0, 0))


def weight_grads(kernel, spread, held, out_shape, out_spec, tile):
    count, width = spread.shape
    return pl.pallas_call(
        kernel,
        grid=(width // tile,),
        out_shape=out_shape,
        in_specs=[pl.BlockSpec((count, tile), lambda i: (0, i))] + [pl.BlockSpec(memory_space=pltpu.VMEM)] * len(held),
        out_specs=out_spec,
        compiler_params=pltpu.CompilerParams(vmem_limit_bytes=vmem_grant),
        cost_estimate=pl.CostEstimate(
            flops=2 * count * sum(math.prod(o.shape) for o in out_shape),
            bytes_accessed=4 * sum(math.prod(o.shape) for o in out_shape),
            transcendentals=0,
        ),
    )(pltpu.with_memory_space_constraint(spread, pltpu.HBM), *held)


def combine_kernel(picks, back, grad_tokens, grad_router):
    ep_count = back.shape[0]
    capacity = picks.shape[1] // ep_count
    rows = jnp.concatenate([back[e, :capacity] for e in range(ep_count)], axis=0)
    grad_tokens[...] = dot(picks[...], rows, (1, 0)).astype(bf16)
    term = back[0, capacity:].astype(f32)
    for e in range(1, ep_count):
        term = term + back[e, capacity:].astype(f32)
    grad_router[...] = term


def on_device(tokens, routes, router, w_gate, w_up, w_down, cotangent):
    ep_count = lax.axis_size("ep")
    tp_count = lax.axis_size("tp")
    tok_rows, width = tokens.shape
    w_gate, w_up, w_down = w_gate[0], w_up[0], w_down[0]
    hidden = w_gate.shape[1]
    experts = router.shape[1]
    capacity = 3 * tok_rows * routes.shape[1] // (2 * experts)
    part, half = width // tp_count, width // cores
    ys = tp_count // cores
    held = ep_count // groups
    count = held * capacity
    wide = round_up(2 * experts, lanes)
    block = power_block(ep_count)
    order = [(turn, flip) for turn in range(ep_count // block) for flip in range(block)]
    to_core = [(i, i ^ 1) for i in range(tp_count)]

    def to_y(step):
        return [(i, (i + step * cores) % tp_count) for i in range(tp_count)]

    def to_ep(step):
        turn, flip = step
        return [(i, (i // block + turn) % (ep_count // block) * block + (i % block ^ flip)) for i in range(ep_count)]

    shapes = [(capacity, wide)] + [(capacity, 2 * half + wide)] * (held - 1)
    shapes += [(2 * part // lanes * capacity + 2 * experts, lanes)] * (ep_count - held)
    dispatch, own_weight, held_tokens, held_cotangent, *blocks = call(
        functools.partial(pack_kernel, order, held, experts, part),
        [shaped((ep_count, capacity, tok_rows), bf16), shaped((capacity, lanes), f32)]
        + [shaped(tokens.shape, bf16), shaped(cotangent.shape, bf16)]
        + [shaped(s, bf16) for s in shapes],
        (tokens, routes.T, router.T, cotangent),
        2 * tok_rows * sum(math.prod(s) for s in shapes),
        [
            pltpu.VMEM(routes.shape[::-1], i32),
            pltpu.VMEM(router.shape[::-1], bf16),
            pltpu.VMEM((wide, tok_rows), f32),
            pltpu.VMEM((wide, tok_rows), f32),
            pltpu.SemaphoreType.DMA((4,)),
        ],
        range(4),
    )
    w_down, picks, own_block = call(
        stage_kernel,
        [shaped(w_down.shape, bf16), shaped((tok_rows, ep_count * capacity), bf16), shaped((capacity, 2 * width), bf16)],
        (w_down, dispatch, own_weight, held_tokens, held_cotangent),
        10**9,
        [pltpu.SemaphoreType.DMA],
        (0,),
    )
    got = [blocks[0]]
    for at in range(1, ep_count):
        got.append(lax.ppermute(blocks[at], "ep", to_ep(order[at])))
    made, terms, sums = (), (), []
    for group in range(groups):
        last = group == groups - 1
        here = got[group * held : (group + 1) * held]
        if group == 0:
            near = jnp.concatenate(here[1:], axis=0)
            sent = (own_block, here[0], near, lax.ppermute(near, "tp", to_core))
        else:
            mine = jnp.concatenate([g[: -2 * experts] for g in here], axis=0)
            meta = jnp.concatenate([g[-2 * experts :] for g in here], axis=0)
            own = [mine] + [lax.ppermute(mine, "tp", to_y(s)) for s in range(1, ys)]
            swapped = [lax.ppermute(own[0], "tp", to_core)]
            swapped += [lax.ppermute(o, "tp", to_core) for o in own[1:]]
            sent = (*own, *swapped, meta)
        outs = [pltpu.HBM((groups * count, width), bf16)] * 2 + [shaped((groups * count, hidden), bf16)] * 3
        outs = outs + [shaped((count + experts if last else count, part), bf16)] * (2 * ys)
        if not last:
            outs = outs + [shaped((experts, part), f32)] * (2 * ys)
        args = (*sent, w_gate, w_up, w_down, router.T, *terms)
        at = len(args)
        got_outs = call(
            functools.partial(expert_kernel, ys, experts, group, last),
            outs,
            (*args, *made),
            10 * count * width * hidden,
            [pltpu.VMEM((count, width), bf16), pltpu.VMEM((count, width), bf16), pltpu.SemaphoreType.DMA((2,))],
            (at, at + 1) if group else (),
            {at + i: i for i in range(5)} if group else None,
            (0, 1),
        )
        made = got_outs[:5]
        terms = got_outs[5 + 2 * ys :]
        keep, give = got_outs[5 : 5 + ys], got_outs[5 + ys : 5 + 2 * ys]
        pairs = [None] * ys
        for step in reversed(range(ys)):
            came = lax.ppermute(give[step], "tp", to_core)
            (pairs[step],) = call(add_kernel, [shaped(came.shape, bf16)], (keep[step], came), came.size)
        sums += [pairs[0]] + [lax.ppermute(pairs[s], "tp", to_y(s)) for s in range(1, ys)]
    (back,) = call(
        functools.partial(return_kernel, order, capacity),
        [shaped((ep_count, capacity + experts, part), bf16)],
        tuple(sums),
        count * part,
    )
    returned = lax.all_to_all(back, "ep", 0, 0, tiled=True)
    rows, cots, act, d_gate, d_up = made
    tile = min(512, width)
    (grad_down,) = weight_grads(
        flat_kernel, cots, (act,), [shaped((hidden, width), f32)],
        [pl.BlockSpec((hidden, tile), lambda i: (0, i))], tile,
    )
    grad_gate, grad_up = weight_grads(
        tall_kernel, rows, (d_gate, d_up), [shaped((width, hidden), f32)] * 2,
        [pl.BlockSpec((tile, hidden), lambda i: (i, 0))] * 2, tile,
    )
    grad_tokens, grad_router = call(
        combine_kernel,
        [shaped((tok_rows, part), bf16), shaped((experts, part), f32)],
        (picks, returned),
        2 * tok_rows * part * capacity * ep_count,
    )
    return (grad_tokens, grad_router.T, grad_gate[None], grad_up[None], grad_down[None])


def solution(mesh):
    return jax.shard_map(
        on_device,
        mesh=mesh,
        in_specs=(
            P("ep", None),
            P("ep", None),
            P(),
            P("ep", None, "tp"),
            P("ep", None, "tp"),
            P("ep", "tp", None),
            P("ep", None),
        ),
        out_specs=(
            P("ep", "tp"),
            P("tp", None),
            P("ep", None, "tp"),
            P("ep", None, "tp"),
            P("ep", "tp", None),
        ),
        check_vma=False,
    )
```
